32 devices in a mesh: sp: 8 (over z, x), tp: 4 (over y, core).
Axes of the slice: x: 2, y: 2, z: 4, core: 2. Of those that a mesh axis runs over, the one named last changes fastest.
Arguments:
- target: bfloat16 [4096, 4096], P(('sp', 'tp')), may hold values from -0.07 to 0.07
- source: bfloat16 [8192, 4096], P(('sp', 'tp')), may hold values from -0.035 to 0.035
- gain_target: float32 [4096], replicated, may hold values from 0.1 to 1.9
- gain_source: float32 [4096], replicated, may hold values from 0.1 to 1.9
- w_query: bfloat16 [4096, 1024], P(None, 'tp'), may hold values from -1 to 1
- w_key: bfloat16 [4096, 512], replicated, may hold values from -1 to 1
- w_value: bfloat16 [4096, 512], replicated, may hold values from -0.09375 to 0.09375
- w_out: bfloat16 [1024, 4096], P('tp'), may hold values from -0.1875 to 0.1875
- grad_output: bfloat16 [4096, 4096], P(('sp', 'tp')), may hold values from -6 to 6
Outputs:
- grad_target: float32 [4096, 4096], P(('sp', 'tp'))
- grad_source: float32 [8192, 4096], P(('sp', 'tp'))
- grad_out_proj: float32 [1024, 4096], P('tp')
The draws below stay inside these ranges and needn't reach their ends.
All inputs are finite; a program needn't handle non-finite values.
Results may differ from the reference program's by a relative error of at most 0.028.
Values may be sent and summed in bfloat16 or wider, within the bound.
A program may use at most 128 MiB of HBM per device.

```python
import jax
import jax.numpy as jnp
from jax import lax

D = 4096
HQ = 16
HK = 8
HD = 64
TGT_ROWS = 4096
SRC_ROWS = 8192


def aligned_draw(key):
    query_weight = jnp.clip(jax.random.normal(jax.random.fold_in(key, 11), (D, HQ * HD), jnp.float32), -6.0, 6.0) * float(D) ** (-0.5)
    key_weight = jnp.clip(jax.random.normal(jax.random.fold_in(key, 12), (D, HK * HD), jnp.float32), -6.0, 6.0) * float(D) ** (-0.5)
    target_rows = jnp.clip(jax.random.normal(jax.random.fold_in(key, 13), (TGT_ROWS, D), jnp.float32), -6.0, 6.0) * 0.01
    source_rows = jnp.clip(jax.random.normal(jax.random.fold_in(key, 14), (SRC_ROWS, D), jnp.float32), -6.0, 6.0) * 0.005
    return (query_weight, key_weight, jnp.clip(target_rows, -0.07, 0.07), jnp.clip(source_rows, -0.035, 0.035))


def draw_target(key, part):
    return aligned_draw(key)[2].astype(jnp.bfloat16)


def draw_source(key, part):
    return aligned_draw(key)[3].astype(jnp.bfloat16)


def draw_w_query(key, part):
    return aligned_draw(key)[0].astype(jnp.bfloat16)


def draw_w_key(key, part):
    return aligned_draw(key)[1].astype(jnp.bfloat16)


def block_levels(stream_key, extent, split, least, largest):
    factor_of, own = 1.0, jax.random.fold_in(stream_key, 6)
    for dim, shards_of in split:
        draws = jnp.exp(jax.random.uniform(jax.random.fold_in(own, dim), (shards_of,), jnp.float32, least / len(split), largest / len(split)))
        factor_of = factor_of * jnp.repeat(draws, extent[dim] // shards_of).reshape([-1 if axis == dim else 1 for axis in range(len(extent))])
    return factor_of


def scatter_about(rng, extent, spread, most, split=(), held_as=jnp.bfloat16):
    factor_of = block_levels(rng, extent, split, -0.22, 0.18) if split else 1.0
    array = jax.random.normal(rng, extent, jnp.float32) * spread * factor_of
    return jnp.minimum(jnp.maximum(array, -most), most).astype(held_as)


def setup_inputs(seed: int = 0) -> dict:
    streams_of = jax.random.split(jax.random.key(seed), 10)
    target = draw_target(jax.random.fold_in(streams_of[9], 71), 0)
    source = draw_source(jax.random.fold_in(streams_of[9], 71), 0)
    gain_target = jnp.clip(1.0 + 0.18 * jax.random.normal(streams_of[2], (D,), jnp.float32), 0.1, 1.9)
    gain_source = jnp.clip(1.0 + 0.18 * jax.random.normal(streams_of[3], (D,), jnp.float32), 0.1, 1.9)
    w_query = draw_w_query(jax.random.fold_in(streams_of[9], 71), 0)
    w_key = draw_w_key(jax.random.fold_in(streams_of[9], 71), 0)
    w_value = scatter_about(streams_of[6], (D, HK * HD), D ** -0.5, 0.09375)
    w_out = scatter_about(streams_of[7], (HQ * HD, D), (HQ * HD) ** -0.5, 0.1875, ((0, 4),))
    grad_output = scatter_about(streams_of[8], (TGT_ROWS, D), 1.0, 6.0, ((0, 32),))
    return dict(target=target, source=source, gain_target=gain_target, gain_source=gain_source, w_query=w_query, w_key=w_key, w_value=w_value, w_out=w_out, grad_output=grad_output)


EPS = 1e-06

def normalize(matrix, scaling):
    widened = matrix.astype(jnp.float32)
    factor = lax.rsqrt(lax.optimization_barrier(jnp.mean(widened * widened, axis=-1, keepdims=True)) + EPS)
    return (widened * factor * scaling.astype(jnp.float32)).astype(jnp.bfloat16)

def norm_back(matrix, scaling, upstream):
    widened = matrix.astype(jnp.float32)
    factor = lax.rsqrt(lax.optimization_barrier(jnp.mean(widened * widened, axis=-1, keepdims=True)) + EPS)
    weighted = upstream * scaling.astype(jnp.float32)
    inner = lax.optimization_barrier(jnp.mean(widened * weighted, axis=-1, keepdims=True))
    return factor * weighted - widened * factor * factor * factor * inner

def reference(target, source, gain_target, gain_source, w_query, w_key, w_value, w_out, grad_output):
    contract_last = (((1,), (1,)), ((), ()))
    normed_target = normalize(target, gain_target)
    normed_source = normalize(source, gain_source)
    query = jnp.dot(normed_target, w_query, preferred_element_type=jnp.float32).astype(jnp.bfloat16)
    keys_all = jnp.dot(normed_source, w_key, preferred_element_type=jnp.float32).astype(jnp.bfloat16)
    values_all = jnp.dot(normed_source, w_value, preferred_element_type=jnp.float32).astype(jnp.bfloat16)
    head_grads = lax.dot_general(grad_output, w_out, contract_last, preferred_element_type=jnp.float32).astype(jnp.bfloat16)
    target_count = target.shape[0]
    source_count = source.shape[0]
    group_size = HQ // HK
    score_scale = float(HD) ** (-0.5)
    query_heads = query.reshape(target_count, HQ, HD).transpose(1, 0, 2)
    grad_heads = head_grads.reshape(target_count, HQ, HD).transpose(1, 0, 2)
    key_heads = keys_all.reshape(source_count, HK, HD).transpose(1, 0, 2)
    value_heads = values_all.reshape(source_count, HK, HD).transpose(1, 0, 2)

    def one_head(bundle):
        query_head, grad_head, position = bundle
        key_head = key_heads[position]
        value_head = value_heads[position]
        scores = jnp.dot(query_head, key_head.T, preferred_element_type=jnp.float32) * score_scale
        maxima = lax.optimization_barrier(jnp.max(scores, axis=-1, keepdims=True))
        weights = jnp.exp(scores - maxima)
        totals = lax.optimization_barrier(jnp.sum(weights, axis=-1, keepdims=True))
        output = (jnp.dot(weights.astype(jnp.bfloat16), value_head, preferred_element_type=jnp.float32) / totals).astype(jnp.bfloat16)
        attend = weights / totals
        delta_sum = lax.optimization_barrier(jnp.sum(grad_head.astype(jnp.float32) * output.astype(jnp.float32), axis=-1, keepdims=True))
        grad_attend = jnp.dot(grad_head, value_head.T, preferred_element_type=jnp.float32)
        mixed = (attend * (grad_attend - delta_sum) * score_scale).astype(jnp.bfloat16)
        grad_query = jnp.dot(mixed, key_head, preferred_element_type=jnp.float32).astype(jnp.bfloat16)
        grad_key = jnp.dot(mixed.T, query_head, preferred_element_type=jnp.float32)
        grad_value = jnp.dot(attend.astype(jnp.bfloat16).T, grad_head, preferred_element_type=jnp.float32)
        return (output, grad_query, grad_key, grad_value)
    positions = jnp.arange(HQ, dtype=jnp.int32) // group_size
    output, grad_query, grad_key, grad_value = lax.map(one_head, (query_heads, grad_heads, positions))
    attention = output.transpose(1, 0, 2).reshape(target_count, HQ * HD)
    query_grads = grad_query.transpose(1, 0, 2).reshape(target_count, HQ * HD)
    key_grads = lax.optimization_barrier(jnp.sum(grad_key.reshape(HK, group_size, source_count, HD), axis=1)).astype(jnp.bfloat16)
    key_grads = key_grads.transpose(1, 0, 2).reshape(source_count, HK * HD)
    value_grads = lax.optimization_barrier(jnp.sum(grad_value.reshape(HK, group_size, source_count, HD), axis=1)).astype(jnp.bfloat16)
    value_grads = value_grads.transpose(1, 0, 2).reshape(source_count, HK * HD)
    grad_xn = lax.dot_general(query_grads, w_query, contract_last, preferred_element_type=jnp.float32)
    grad_target = norm_back(target, gain_target, grad_xn)
    grad_sn = lax.dot_general(key_grads, w_key, contract_last, preferred_element_type=jnp.float32)
    grad_sn = grad_sn + lax.dot_general(value_grads, w_value, contract_last, preferred_element_type=jnp.float32)
    grad_source = norm_back(source, gain_source, grad_sn)
    grad_out_proj = lax.dot_general(attention, grad_output, (((0,), (0,)), ((), ())), preferred_element_type=jnp.float32)
    return (grad_target, grad_source, grad_out_proj)
```

```python
import functools
import math

import jax
import jax.numpy as jnp
from jax import lax
from jax.experimental import pallas as pl
from jax.experimental.pallas import tpu as pltpu
from jax.sharding import PartitionSpec as P

HD = 64
BLOCK = 512
LIMIT = 63000 * 1024


EPS = 1e-06


def normalize(matrix, scaling):
    widened = matrix.astype(jnp.float32)
    factor = lax.rsqrt(jnp.mean(widened * widened, axis=-1, keepdims=True) + EPS)
    return (widened * factor * scaling).astype(jnp.bfloat16)


def norm_back(matrix, scaling, upstream):
    widened = matrix.astype(jnp.float32)
    factor = lax.rsqrt(jnp.mean(widened * widened, axis=-1, keepdims=True) + EPS)
    weighted = upstream * scaling
    inner = jnp.mean(widened * weighted, axis=-1, keepdims=True)
    return factor * weighted - widened * factor * factor * factor * inner


def attend_kernel(key_count, group_size, block, q_ref, d_ref, kv_ref, o_ref, dq_ref, dkv_ref,
                  qpad, dpad, kvt, estore, mstore, ot, dqt):
    rows = q_ref.shape[0]
    width = kv_ref.shape[1]
    half = key_count * HD
    cols = group_size * rows
    blocks = kv_ref.shape[0] // block
    scale = float(HD) ** (-0.5)
    nt = (((1,), (1,)), ((), ()))
    nn = (((1,), (0,)), ((), ()))
    f32 = jnp.float32
    lane = lax.broadcasted_iota(jnp.int32, (rows, width), 1)
    qf = q_ref[...].astype(f32) * scale
    df = d_ref[...].astype(f32)
    if qf.shape[1] < width:
        qf = jnp.concatenate([qf] * (width // qf.shape[1]), axis=1)
        df = jnp.concatenate([df] * (width // df.shape[1]), axis=1)
    dt = d_ref[...].astype(f32).T
    for g in range(key_count):
        for j in range(group_size):
            h = g * group_size + j
            for source, store, base in ((qf, qpad, g * HD), (df, dpad, half + g * HD)):
                turn = (base - h * HD) % width
                moved = pltpu.roll(source, turn, 1) if turn else source
                keep = (lane >= base) & (lane < base + HD)
                store[g, j * rows:(j + 1) * rows, :] = jnp.where(keep, moved, 0.0).astype(jnp.bfloat16)

    def advance(i, state):
        here = pl.ds(pl.multiple_of(i * block, block), block)
        kvb = kv_ref[here, :]
        kvbt = kvb.astype(f32).T.astype(jnp.bfloat16)
        kvt[:, here] = kvbt
        out = []
        for g in range(key_count):
            m, l = state[2 * g], state[2 * g + 1]
            s = lax.dot_general(kvb, qpad[g], nt, preferred_element_type=f32)
            m_new = jnp.maximum(m, jnp.max(s, axis=0, keepdims=True))
            shrink = jnp.exp(m - m_new)
            e = jnp.exp(s - m_new)
            eb = e.astype(jnp.bfloat16)
            estore[g, here, :] = eb
            mstore[g, pl.ds(i, 1), :] = m_new
            l = l * shrink + jnp.sum(e, axis=0, keepdims=True)
            vt = kvbt[half + g * HD:half + (g + 1) * HD, :]
            ot[g] = ot[g] * shrink + lax.dot_general(vt, eb, nn, preferred_element_type=f32)
            out += [m_new, l]
        return tuple(out)

    ot[...] = jnp.zeros_like(ot)
    dqt[...] = jnp.zeros_like(dqt)
    start = []
    for g in range(key_count):
        start += [jnp.full((1, cols), -jnp.inf, f32), jnp.zeros((1, cols), f32)]
    state = lax.fori_loop(0, blocks, advance, tuple(start))

    deltas = []
    for g in range(key_count):
        inv = 1.0 / state[2 * g + 1]
        og = (ot[g] * inv).astype(jnp.bfloat16)
        ot[g] = og.astype(f32)
        parts = []
        for j in range(group_size):
            h = g * group_size + j
            parts.append(jnp.sum(dt[h * HD:(h + 1) * HD, :] * ot[g, :, j * rows:(j + 1) * rows], axis=0, keepdims=True))
        deltas.append(jnp.concatenate(parts, axis=1))
        mstore[g] = jnp.exp(mstore[g] - state[2 * g]) * inv
    pieces = [ot[g, :, j * rows:(j + 1) * rows] for g in range(key_count) for j in range(group_size)]
    o_ref[...] = jnp.concatenate(pieces, axis=0).T.astype(jnp.bfloat16)

    def collect(i, carry):
        here = pl.ds(pl.multiple_of(i * block, block), block)
        kvb = kv_ref[here, :]
        total = jnp.zeros((block, width), f32)
        for g in range(key_count):
            dp = lax.dot_general(kvb, dpad[g], nt, preferred_element_type=f32)
            p = estore[g, here, :].astype(f32) * mstore[g, pl.ds(i, 1), :]
            mixed = (p * (dp - deltas[g])).astype(jnp.bfloat16)
            total = total + lax.dot_general(mixed, qpad[g], nn, preferred_element_type=f32)
            total = total + lax.dot_general(p.astype(jnp.bfloat16), dpad[g], nn, preferred_element_type=f32)
            kt = kvt[g * HD:(g + 1) * HD, here]
            dqt[g] += lax.dot_general(kt, mixed, nn, preferred_element_type=f32)
        dkv_ref[here, :] = total.astype(jnp.bfloat16)
        return carry

    lax.fori_loop(0, blocks, collect, 0)
    pieces = [dqt[g, :, j * rows:(j + 1) * rows] for g in range(key_count) for j in range(group_size)]
    dq_ref[...] = (jnp.concatenate(pieces, axis=0) * scale).T.astype(jnp.bfloat16)


def attend(queries, grads, pairs, key_count, group_size):
    rows = queries.shape[0]
    source_rows, width = pairs.shape
    cols = group_size * rows
    block = math.gcd(source_rows, BLOCK)
    bf16, f32 = jnp.bfloat16, jnp.float32
    work = source_rows * cols * key_count * HD * 2
    whole = pl.BlockSpec(memory_space=pltpu.VMEM)
    return pl.pallas_call(
        functools.partial(attend_kernel, key_count, group_size, block),
        out_shape=(
            jax.ShapeDtypeStruct(queries.shape, bf16),
            jax.ShapeDtypeStruct(queries.shape, bf16),
            jax.ShapeDtypeStruct(pairs.shape, bf16),
        ),
        in_specs=[whole] * 3,
        out_specs=(whole,) * 3,
        scratch_shapes=[
            pltpu.VMEM((key_count, cols, width), bf16),
            pltpu.VMEM((key_count, cols, width), bf16),
            pltpu.VMEM((width, source_rows), bf16),
            pltpu.VMEM((key_count, source_rows, cols), bf16),
            pltpu.VMEM((key_count, source_rows // block, cols), f32),
            pltpu.VMEM((key_count, HD, cols), f32),
            pltpu.VMEM((key_count, HD, cols), f32),
        ],
        compiler_params=pltpu.CompilerParams(vmem_limit_bytes=LIMIT),
        cost_estimate=pl.CostEstimate(flops=6 * 4 * work, bytes_accessed=10 << 20, transcendentals=0),
        name="attend",
    )(queries, grads, pairs)


def shards(target, source, gain_target, gain_source, w_query, w_key, w_value, w_out, grad_output):
    contract_last = (((1,), (1,)), ((), ()))
    across = lax.axis_size("tp")
    heads_all = w_key.shape[1] // HD
    key_count = heads_all // across
    query_count = w_query.shape[1] // HD
    group_size = query_count // key_count
    normed_target = normalize(target, gain_target)
    normed_source = normalize(source, gain_source)
    gathered_target, gathered_grad = (
        lax.all_gather(normed_target, "tp", axis=0, tiled=True),
        lax.all_gather(grad_output, "tp", axis=0, tiled=True),
    )
    query = jnp.dot(gathered_target, w_query, preferred_element_type=jnp.float32).astype(
        jnp.bfloat16
    )
    head_grads = lax.dot_general(
        gathered_grad, w_out, contract_last, preferred_element_type=jnp.float32
    ).astype(jnp.bfloat16)
    keys_part = jnp.dot(normed_source, w_key, preferred_element_type=jnp.float32).astype(jnp.bfloat16)
    values_part = jnp.dot(normed_source, w_value, preferred_element_type=jnp.float32).astype(
        jnp.bfloat16
    )
    source_count = source.shape[0]
    pairs = jnp.concatenate(
        [
            keys_part.reshape(source_count, across, key_count * HD),
            values_part.reshape(source_count, across, key_count * HD),
        ],
        axis=2,
    ).reshape(source_count, across * 2 * key_count * HD)
    own_pairs = lax.all_to_all(pairs, "tp", split_axis=1, concat_axis=0, tiled=True)
    all_pairs = lax.all_gather(own_pairs, "sp", axis=0, tiled=True)
    attention, grad_query, pair_store = attend(query, head_grads, all_pairs, key_count, group_size)
    pair_grads = lax.psum_scatter(
        pair_store, "sp", scatter_dimension=0, tiled=True
    )
    pair_rows = lax.all_to_all(pair_grads, "tp", split_axis=0, concat_axis=1, tiled=True)
    split_rows = pair_rows.reshape(source_count, across, 2, key_count * HD)
    key_grads = split_rows[:, :, 0].reshape(source_count, heads_all * HD)
    value_grads = split_rows[:, :, 1].reshape(source_count, heads_all * HD)
    grad_sn = lax.dot_general(key_grads, w_key, contract_last, preferred_element_type=jnp.float32)
    grad_sn = grad_sn + lax.dot_general(
        value_grads, w_value, contract_last, preferred_element_type=jnp.float32
    )
    grad_source = norm_back(source, gain_source, grad_sn)
    proj_part = lax.dot_general(
        attention, gathered_grad, (((0,), (0,)), ((), ())), preferred_element_type=jnp.float32
    )
    grad_out_proj = lax.psum(proj_part.astype(jnp.bfloat16), "sp").astype(jnp.float32)
    grad_xn = lax.psum_scatter(
        lax.dot_general(
            grad_query, w_query, contract_last, preferred_element_type=jnp.float32
        ).astype(jnp.bfloat16),
        "tp",
        scatter_dimension=0,
        tiled=True,
    ).astype(jnp.float32)
    grad_target = norm_back(target, gain_target, grad_xn)
    return (grad_target, grad_source, grad_out_proj)


def solution(mesh):
    return jax.shard_map(
        shards,
        mesh=mesh,
        in_specs=(
            P(("sp", "tp"), None),
            P(("sp", "tp"), None),
            P(),
            P(),
            P(None, "tp"),
            P(),
            P(),
            P("tp", None),
            P(("sp", "tp"), None),
        ),
        out_specs=(P(("sp", "tp"), None), P(("sp", "tp"), None), P("tp", None)),
        check_vma=False,
    )
```

```python
import functools
import math

import jax
import jax.numpy as jnp
from jax import lax
from jax.experimental import pallas as pl
from jax.experimental.pallas import tpu as pltpu
from jax.sharding import PartitionSpec as P

HD = 64
BLOCK = 512
LIMIT = 63000 * 1024


EPS = 1e-06


def normalize(matrix, scaling):
    widened = matrix.astype(jnp.float32)
    factor = lax.rsqrt(jnp.mean(widened * widened, axis=-1, keepdims=True) + EPS)
    return (widened * factor * scaling).astype(jnp.bfloat16)


def norm_back(matrix, scaling, upstream):
    widened = matrix.astype(jnp.float32)
    factor = lax.rsqrt(jnp.mean(widened * widened, axis=-1, keepdims=True) + EPS)
    weighted = upstream * scaling
    inner = jnp.mean(widened * weighted, axis=-1, keepdims=True)
    return factor * weighted - widened * factor * factor * factor * inner


def attend_kernel(key_count, group_size, block, q_ref, d_ref, kv_ref, o_ref, dq_ref, dkv_ref,
                  qpad, dpad, kvt, estore, mstore, ot, dqt):
    rows = q_ref.shape[0]
    width = kv_ref.shape[1]
    half = key_count * HD
    cols = group_size * rows
    blocks = kv_ref.shape[0] // block
    scale = float(HD) ** (-0.5)
    nt = (((1,), (1,)), ((), ()))
    nn = (((1,), (0,)), ((), ()))
    f32 = jnp.float32
    lane = lax.broadcasted_iota(jnp.int32, (rows, width), 1)
    qf = q_ref[...].astype(f32) * scale
    df = d_ref[...].astype(f32)
    if qf.shape[1] < width:
        qf = jnp.concatenate([qf] * (width // qf.shape[1]), axis=1)
        df = jnp.concatenate([df] * (width // df.shape[1]), axis=1)
    dt = d_ref[...].astype(f32).T
    for g in range(key_count):
        for j in range(group_size):
            h = g * group_size + j
            for source, store, base in ((qf, qpad, g * HD), (df, dpad, half + g * HD)):
                turn = (base - h * HD) % width
                moved = pltpu.roll(source, turn, 1) if turn else source
                keep = (lane >= base) & (lane < base + HD)
                store[g, j * rows:(j + 1) * rows, :] = jnp.where(keep, moved, 0.0).astype(jnp.bfloat16)

    def advance(i, state):
        here = pl.ds(pl.multiple_of(i * block, block), block)
        kvb = kv_ref[here, :]
        kvbt = kvb.astype(f32).T.astype(jnp.bfloat16)
        kvt[:, here] = kvbt
        out = []
        for g in range(key_count):
            m, l = state[2 * g], state[2 * g + 1]
            s = lax.dot_general(kvb, qpad[g], nt, preferred_element_type=f32)
            m_new = jnp.maximum(m, jnp.max(s, axis=0, keepdims=True))
            shrink = jnp.exp(m - m_new)
            e = jnp.exp(s - m_new)
            eb = e.astype(jnp.bfloat16)
            estore[g, here, :] = eb
            mstore[g, pl.ds(i, 1), :] = m_new
            l = l * shrink + jnp.sum(e, axis=0, keepdims=True)
            vt = kvbt[half + g * HD:half + (g + 1) * HD, :]
            ot[g] = ot[g] * shrink + lax.dot_general(vt, eb, nn, preferred_element_type=f32)
            out += [m_new, l]
        return tuple(out)

    ot[...] = jnp.zeros_like(ot)
    dqt[...] = jnp.zeros_like(dqt)
    start = []
    for g in range(key_count):
        start += [jnp.full((1, cols), -jnp.inf, f32), jnp.zeros((1, cols), f32)]
    state = lax.fori_loop(0, blocks, advance, tuple(start))

    deltas = []
    for g in range(key_count):
        inv = 1.0 / state[2 * g + 1]
        og = (ot[g] * inv).astype(jnp.bfloat16)
        ot[g] = og.astype(f32)
        parts = []
        for j in range(group_size):
            h = g * group_size + j
            parts.append(jnp.sum(dt[h * HD:(h + 1) * HD, :] * ot[g, :, j * rows:(j + 1) * rows], axis=0, keepdims=True))
        deltas.append(jnp.concatenate(parts, axis=1))
        mstore[g] = jnp.exp(mstore[g] - state[2 * g]) * inv
    pieces = [ot[g, :, j * rows:(j + 1) * rows] for g in range(key_count) for j in range(group_size)]
    o_ref[...] = jnp.concatenate(pieces, axis=0).T.astype(jnp.bfloat16)

    def collect(i, carry):
        here = pl.ds(pl.multiple_of(i * block, block), block)
        kvb = kv_ref[here, :]
        total = jnp.zeros((block, width), f32)
        for g in range(key_count):
            dp = lax.dot_general(kvb, dpad[g], nt, preferred_element_type=f32)
            p = estore[g, here, :].astype(f32) * mstore[g, pl.ds(i, 1), :]
            mixed = (p * (dp - deltas[g])).astype(jnp.bfloat16)
            total = total + lax.dot_general(mixed, qpad[g], nn, preferred_element_type=f32)
            total = total + lax.dot_general(p.astype(jnp.bfloat16), dpad[g], nn, preferred_element_type=f32)
            kt = kvt[g * HD:(g + 1) * HD, here]
            dqt[g] += lax.dot_general(kt, mixed, nn, preferred_element_type=f32)
        dkv_ref[here, :] = total.astype(jnp.bfloat16)
        return carry

    lax.fori_loop(0, blocks, collect, 0)
    pieces = [dqt[g, :, j * rows:(j + 1) * rows] for g in range(key_count) for j in range(group_size)]
    dq_ref[...] = (jnp.concatenate(pieces, axis=0) * scale).T.astype(jnp.bfloat16)


def attend(queries, grads, pairs, key_count, group_size):
    rows = queries.shape[0]
    source_rows, width = pairs.shape
    cols = group_size * rows
    block = math.gcd(source_rows, BLOCK)
    bf16, f32 = jnp.bfloat16, jnp.float32
    work = source_rows * cols * key_count * HD * 2
    whole = pl.BlockSpec(memory_space=pltpu.VMEM)
    return pl.pallas_call(
        functools.partial(attend_kernel, key_count, group_size, block),
        out_shape=(
            jax.ShapeDtypeStruct(queries.shape, bf16),
            jax.ShapeDtypeStruct(queries.shape, bf16),
            jax.ShapeDtypeStruct(pairs.shape, bf16),
        ),
        in_specs=[whole] * 3,
        out_specs=(whole,) * 3,
        scratch_shapes=[
            pltpu.VMEM((key_count, cols, width), bf16),
            pltpu.VMEM((key_count, cols, width), bf16),
            pltpu.VMEM((width, source_rows), bf16),
            pltpu.VMEM((key_count, source_rows, cols), bf16),
            pltpu.VMEM((key_count, source_rows // block, cols), f32),
            pltpu.VMEM((key_count, HD, cols), f32),
            pltpu.VMEM((key_count, HD, cols), f32),
        ],
        compiler_params=pltpu.CompilerParams(vmem_limit_bytes=LIMIT),
        cost_estimate=pl.CostEstimate(flops=6 * 4 * work, bytes_accessed=10 << 20, transcendentals=0),
        name="attend",
    )(queries, grads, pairs)


def swap(block, axis, mask):
    pairs = [(i, i ^ mask) for i in range(lax.axis_size(axis))]
    return lax.ppermute(block, axis, pairs)


def spread(block, axis, stages):
    held = {0: block}
    for masks in stages:
        grown = dict(held)
        for mask in masks:
            for r in held:
                grown[r ^ mask] = swap(held[r], axis, mask)
        held = grown
    return held


def combine(parts, axis, stages):
    total = None
    for masks in stages:
        span = 0
        for mask in masks:
            span |= mask
        kept = {}
        for r in parts:
            if r & span:
                continue
            total = parts[r].astype(jnp.float32)
            for mask in masks:
                total = total + swap(parts[r ^ mask], axis, mask).astype(jnp.float32)
            kept[r] = total.astype(jnp.bfloat16)
        parts = kept
    return total


def in_order(held, axis):
    stacked = jnp.stack([held[r] for r in range(len(held))])
    me = lax.axis_index(axis)
    return [lax.dynamic_index_in_dim(stacked, me ^ j, 0, keepdims=False) for j in range(len(held))]


def shards(target, source, gain_target, gain_source, w_query, w_key, w_value, w_out, grad_output):
    contract_last = (((1,), (1,)), ((), ()))
    across, around = lax.axis_size("tp"), lax.axis_size("sp")
    my_tp, my_sp = lax.axis_index("tp"), lax.axis_index("sp")
    chips = [list(range(2, across, 2)), [1]]
    inner = 1 << ((around.bit_length() - 1) // 2)
    near, far = list(range(1, inner)), list(range(inner, around, inner))
    routes = ([near, far], [far, near])
    heads_all = w_key.shape[1] // HD
    key_count = heads_all // across
    query_count = w_query.shape[1] // HD
    group_size = query_count // key_count
    f32, bf16 = jnp.float32, jnp.bfloat16

    normed_source = normalize(source, gain_source)
    keys_part = jnp.dot(normed_source, w_key, preferred_element_type=f32).astype(bf16)
    values_part = jnp.dot(normed_source, w_value, preferred_element_type=f32).astype(bf16)
    source_count = source.shape[0]
    pairs = jnp.concatenate(
        [
            keys_part.reshape(source_count, across, key_count * HD),
            values_part.reshape(source_count, across, key_count * HD),
        ],
        axis=2,
    )
    own = []
    for r in range(across):
        piece = lax.dynamic_index_in_dim(pairs, my_tp ^ r, 1, keepdims=False)
        own.append(swap(piece, "tp", r) if r else piece)
    halves = (
        jnp.concatenate(own[: across // 2], axis=0),
        jnp.concatenate(own[across // 2 :], axis=0),
    )
    arrived = [spread(half, "sp", route) for half, route in zip(halves, routes)]
    all_pairs = jnp.concatenate([arrived[s][r] for r in range(around) for s in range(2)], axis=0)

    normed_target = normalize(target, gain_target)
    targets = spread(normed_target, "tp", chips)
    grads = spread(grad_output, "tp", chips)
    query = jnp.concatenate(
        [jnp.dot(targets[r], w_query, preferred_element_type=f32).astype(bf16) for r in range(across)],
        axis=0,
    )
    head_grads = jnp.concatenate(
        [
            lax.dot_general(grads[r], w_out, contract_last, preferred_element_type=f32).astype(bf16)
            for r in range(across)
        ],
        axis=0,
    )
    gathered_grad = jnp.concatenate([grads[r] for r in range(across)], axis=0)

    attention, grad_query, pair_store = attend(query, head_grads, all_pairs, key_count, group_size)

    half_rows = halves[0].shape[0]
    owned = []
    for s, route in enumerate(routes):
        parts = {}
        for r in range(around):
            begin = (2 * r + s) * half_rows
            parts[r] = pair_store[begin : begin + half_rows]
        owned.append(combine(parts, "sp", route[::-1]).astype(bf16))
    returned = {}
    for r in range(across):
        part = owned[r // (across // 2)]
        begin = (r % (across // 2)) * source_count
        piece = part[begin : begin + source_count]
        returned[r] = swap(piece, "tp", r) if r else piece
    ordered = in_order(returned, "tp")
    cut = key_count * HD
    key_grads = jnp.concatenate([piece[:, :cut] for piece in ordered], axis=1)
    value_grads = jnp.concatenate([piece[:, cut:] for piece in ordered], axis=1)
    grad_sn = lax.dot_general(key_grads, w_key, contract_last, preferred_element_type=f32)
    grad_sn = grad_sn + lax.dot_general(
        value_grads, w_value, contract_last, preferred_element_type=f32
    )
    grad_source = norm_back(source, gain_source, grad_sn)

    row_count = target.shape[0]
    parts = {}
    for r in range(across):
        rows = grad_query[r * row_count : (r + 1) * row_count]
        parts[r] = lax.dot_general(rows, w_query, contract_last, preferred_element_type=f32).astype(bf16)
    grad_xn = combine(parts, "tp", chips[::-1])
    grad_target = norm_back(target, gain_target, grad_xn)

    proj_part = lax.dot_general(
        attention, gathered_grad, (((0,), (0,)), ((), ())), preferred_element_type=f32
    ).astype(bf16)
    share = proj_part.shape[0] // around
    middle = proj_part.shape[1] // 2
    columns = []
    for s, route in enumerate(routes):
        parts = {}
        for r in range(around):
            rows = lax.dynamic_slice_in_dim(proj_part, (my_sp ^ r) * share, share, 0)
            parts[r] = rows[:, s * middle : (s + 1) * middle]
        mine = combine(parts, "sp", route[::-1]).astype(bf16)
        held = spread(mine, "sp", route)
        columns.append(jnp.concatenate(in_order(held, "sp"), axis=0))
    grad_out_proj = jnp.concatenate(columns, axis=1).astype(f32)
    return (grad_target, grad_source, grad_out_proj)


def solution(mesh):
    return jax.shard_map(
        shards,
        mesh=mesh,
        in_specs=(
            P(("sp", "tp"), None),
            P(("sp", "tp"), None),
            P(),
            P(),
            P(None, "tp"),
            P(),
            P(),
            P("tp", None),
            P(("sp", "tp"), None),
        ),
        out_specs=(P(("sp", "tp"), None), P(("sp", "tp"), None), P("tp", None)),
        check_vma=False,
    )
```
